256 devices in a mesh: grp: 4 (over y, x), ep: 64 (over z, core).
Axes of the slice: x: 2, y: 2, z: 32, core: 2. Of those that a mesh axis runs over, the one named last changes fastest.
The devices are a block of a 4x8x32 slice.
Arguments:
- tokens: bfloat16 [32768, 2048], P(('grp', 'ep')), parts along dimension 0, may hold values from -6 to 6
- routing: int32 [32768, 2], P(('grp', 'ep')), parts along dimension 0, may hold values from 0 to 15, all different within a row; in each aligned block of 128 rows (0 to 127, 128 to 255, ...) at most 20 rows name the same one
- gates: float32 [32768, 2], P(('grp', 'ep')), parts along dimension 0, may hold values from 0.2 to 1
- norm_gain: bfloat16 [2048], replicated, may hold values from 0.099609375 to 1.8984375
- w_gate: bfloat16 [64, 2048, 896], P('ep'), may hold values from -0.125 to 0.125
- w_up: bfloat16 [64, 2048, 896], P('ep'), may hold values from -0.125 to 0.125
- w_down: bfloat16 [64, 896, 2048], P('ep'), may hold values from -0.09375 to 0.09375
Outputs:
- mixed: bfloat16 [32768, 2048], P(('grp', 'ep')), parts along dimension 0
The draws below stay inside these ranges and needn't reach their ends.
There are 4 independent parts, one for each index of `grp`. The reference program is written for one: setup_inputs(seed, part) draws one part's arguments, and reference() takes and returns one part's arrays. A program takes and returns all parts, laid end to end along the dimension named above; an argument that names none is the same for every part. Nothing has to cross between parts.
Inputs may be any that keep to these rules, and one draw needn't show every extreme that they name: `routing`: each row names 2 different experts. Among the rows of one device at most 20 name any one expert, and in every draw some expert is named by exactly 20 rows of some device.
All inputs are finite; a program needn't handle non-finite values.
Results may differ from the reference program's by a relative error of at most 0.0078.
Values may be sent and summed in bfloat16 or wider, within the bound.
A program may use at most 128 MiB of HBM per device.

```python
import math
import jax
import jax.numpy as jnp
import numpy as np
from jax import lax

D = 2048
FF = 3584
TOP = 2
GROUP = 4
TOK_DEV = 128
EXPERTS = 16
CAP = 20
TOKENS = 8192
N_EP = 64


def levels(key, dims, pieces, low, top_value):
    factor_of, own = 1.0, jax.random.fold_in(key, 6)
    for axis_at, blocks in pieces:
        steps = jnp.exp(jax.random.uniform(jax.random.fold_in(own, axis_at), (blocks,), jnp.float32, low / len(pieces), top_value / len(pieces)))
        factor_of = factor_of * jnp.repeat(steps, dims[axis_at] // blocks).reshape([-1 if axis == axis_at else 1 for axis in range(len(dims))])
    return factor_of


def assign_block(own_key, own, number, rows, number_of, top, bound, lean):
    order = jax.random.permutation(own_key, number_of)
    heavy_load, common = load_shares(number_of, rows * top, bound, lean, True), load_shares(number_of, rows * top, bound, lean, False)
    places = jnp.arange(number_of)

    def named(sizes, offset_by):
        used = int((sizes > 0).sum())
        fixed = max(1, used // 4)
        passed = fixed + (places - fixed + offset_by * (used - fixed)) % max(1, number_of - fixed)
        return jnp.zeros((number_of,), jnp.int32).at[order[jnp.where(places < fixed, places, passed)]].set(jnp.asarray(sizes, jnp.int32))

    sizes = jnp.where(number % 4 == 0, named(heavy_load, number // 4), named(common, number - number // 4 - 1))
    mixed = jax.random.permutation(jax.random.fold_in(own, 3), number_of)
    donor, taker = mixed[0:number_of // 2 * 2:2], mixed[1:number_of // 2 * 2:2]
    room = jnp.minimum(sizes[donor] - 1, bound - sizes[taker]) // 2
    room = jnp.where((donor == order[0]) | (taker == order[0]) | (sizes[taker] == 0), 0, jnp.maximum(room, 0))
    passed = jax.random.randint(jax.random.fold_in(own, 4), (number_of // 2,), 0, 1 << 20) % (room + 1)
    sizes = sizes.at[donor].add(-passed).at[taker].add(passed)
    labels = jnp.searchsorted(jnp.cumsum(sizes), jnp.arange(rows * top), side="right").astype(jnp.int32)
    table = labels.reshape(top, rows).T
    table = table[jax.random.permutation(jax.random.fold_in(own, 1), rows)]
    offset_by = jax.random.randint(jax.random.fold_in(own, 2), (rows, 1), 0, top)
    return jnp.take_along_axis(table, (jnp.arange(top)[None, :] + offset_by) % top, axis=1)


def load_shares(number_of, total, bound, skew, full):
    portions = [(1 << 20) // math.isqrt(grade ** skew) + 1 for grade in range(1, number_of + 1)]
    largest = bound if full else min(bound, max(-(-total // number_of), total * portions[0] // sum(portions)))
    least = 1 if total - largest >= number_of - 1 else 0
    given, spare = [largest] + [least] * (number_of - 1), total - largest - least * (number_of - 1)
    while spare > 0:
        free = [i for i in range(1, number_of) if given[i] < largest] or [i for i in range(1, number_of) if given[i] < bound]
        pool, left = sum([portions[i] for i in free]), spare
        for i in free:
            extra = min(bound - given[i], max(1, left * portions[i] // pool), spare)
            given[i] = given[i] + extra
            spare = spare - extra
    return np.array(given)


def normal_values(rng, shape, deviation, limit, pieces=(), kind=jnp.bfloat16):
    values = deviation * jax.random.normal(rng, shape, jnp.float32)
    if pieces:
        values = values * levels(rng, shape, pieces, -0.22, 0.18)
    return jnp.clip(values, -limit, limit).astype(kind)


def setup_inputs(seed: int = 0, part: int = 0) -> dict:
    key_of = jax.random.split(jax.random.key(seed), 8)
    own_keys = jax.random.split(jax.random.fold_in(key_of[7], part), 8)
    tokens = normal_values(own_keys[0], (TOKENS, D), 1.0, 6.0, ((0, 64),))
    routing_keys = jax.random.split(jax.random.fold_in(own_keys[1], 1), TOKENS // TOK_DEV)
    routing_turns = jax.random.permutation(jax.random.fold_in(own_keys[1], 3), TOKENS // TOK_DEV)
    routing = jax.vmap(lambda own, number: assign_block(jax.random.fold_in(own_keys[1], 2), own, number, TOK_DEV, EXPERTS, TOP, CAP, 2))(routing_keys, routing_turns).reshape((TOKENS, TOP))
    gates = jnp.clip(0.2 + 0.8 * jax.random.uniform(own_keys[2], (TOKENS, TOP), jnp.float32) ** levels(own_keys[2], (TOKENS, TOP), ((0, 64),), -0.2, 0.2), 0.2, 1.0)
    norm_gain = jnp.clip(1.0 + 0.18 * jax.random.normal(key_of[3], (D,), jnp.float32), 0.099609375, 1.8984375).astype(jnp.bfloat16)
    w_gate = normal_values(key_of[4], (N_EP, D, FF // GROUP), D ** -0.5, 0.125, ((0, 64),))
    w_up = normal_values(key_of[5], (N_EP, D, FF // GROUP), D ** -0.5, 0.125, ((0, 64),))
    w_down = normal_values(key_of[6], (N_EP, FF // GROUP, D), FF ** -0.5, 0.09375, ((0, 64),))
    return dict(tokens=tokens, routing=routing, gates=gates, norm_gain=norm_gain, w_gate=w_gate, w_up=w_up, w_down=w_down)


def run_expert(operands):
    expert_rows, gate_piece, up_piece, down_piece = operands
    gate_matrix = jnp.moveaxis(gate_piece, 0, 1).reshape(D, FF)
    up_matrix = jnp.moveaxis(up_piece, 0, 1).reshape(D, FF)
    gate_act = jnp.dot(expert_rows, gate_matrix, preferred_element_type=jnp.float32)
    up_act = jnp.dot(expert_rows, up_matrix, preferred_element_type=jnp.float32)
    hidden = (jax.nn.silu(gate_act) * up_act).astype(jnp.bfloat16)
    return jnp.dot(hidden, down_piece, preferred_element_type=jnp.float32).astype(jnp.bfloat16)

def reference(tokens, routing, gates, norm_gain, w_gate, w_up, w_down):
    values = tokens.astype(jnp.float32)
    scale = lax.rsqrt(lax.optimization_barrier(jnp.mean(values * values, axis=-1, keepdims=True)) + 1e-06)
    normed = (values * scale * norm_gain.astype(jnp.float32)).astype(jnp.bfloat16)
    blocks = routing.reshape(N_EP, TOK_DEV, TOP).astype(jnp.int32)
    one_hot = (blocks[..., None] == jnp.arange(EXPERTS, dtype=jnp.int32)).astype(jnp.int32)
    per_token = lax.optimization_barrier(jnp.sum(one_hot, axis=2)).astype(jnp.int32)
    before = (jnp.cumsum(per_token, axis=1) - per_token).astype(jnp.int32)
    slots = lax.optimization_barrier(jnp.sum(one_hot * before[:, :, None, :], axis=-1)).astype(jnp.int32)
    source = jnp.arange(N_EP, dtype=jnp.int32)[:, None, None]
    target = ((blocks * N_EP + source) * CAP + slots).reshape(-1).astype(jnp.int32)
    filled = jnp.zeros((EXPERTS * N_EP * CAP, D), jnp.bfloat16)
    filled = filled.at[target].set(jnp.repeat(normed, TOP, axis=0))
    expert_rows = filled.reshape(EXPERTS, N_EP * CAP, D)
    gate_pieces = w_gate.reshape(EXPERTS, GROUP, D, FF // GROUP)
    up_pieces = w_up.reshape(EXPERTS, GROUP, D, FF // GROUP)
    down_pieces = w_down.reshape(EXPERTS, FF, D)
    results = lax.map(run_expert, (expert_rows, gate_pieces, up_pieces, down_pieces))
    picked = results.reshape(EXPERTS * N_EP * CAP, D)[target].reshape(N_EP * TOK_DEV, TOP, D)
    mixed = lax.optimization_barrier(jnp.sum(gates[..., None] * picked.astype(jnp.float32), axis=1))
    return mixed.astype(jnp.bfloat16)
```

```python
import functools

import jax
import jax.numpy as jnp
from jax import lax
from jax.experimental import pallas as pl
from jax.experimental.pallas import tpu as pltpu
from jax.sharding import PartitionSpec as P

GROUP = 4
SUB = 16
WINDOW = 2
F32, BF16 = jnp.float32, jnp.bfloat16


def dot(a, b):
    return jnp.dot(a, b, preferred_element_type=F32)


def iota(shape, dim):
    return lax.broadcasted_iota(jnp.int32, shape, dim)


def layer_kernel(
    devices,
    cap,
    tokens_ref,
    routing_ref,
    gates_ref,
    gain_ref,
    wg_hbm,
    wu_hbm,
    wd_hbm,
    out_ref,
    wg,
    wu,
    wd,
    normed,
    target,
    weight,
    outgoing,
    mine,
    theirs,
    rows,
    hidden,
    kept,
    given,
    part,
    final,
    returned,
    w_sem,
    w_send,
    w_recv,
    d_send,
    d_recv,
    l_send,
    l_recv,
    p_send,
    p_recv,
    r_send,
    r_recv,
):
    tok, width = tokens_ref.shape
    ff = wg_hbm.shape[2]
    extra = cap - SUB
    folds = SUB // extra
    part_w = width // folds
    experts = devices // GROUP
    steps = experts // 2

    me = lax.axis_index("ep")
    core = me % 2
    pair = me // GROUP
    role = me // 2 % 2
    mate = me + 2 - 4 * role
    twin = me + 1 - 2 * core

    def device_of(pair_at, role_at):
        return lax.rem(pair_at + 2 * experts, experts) * GROUP + role_at * 2 + core

    def delta_of(step):
        return lax.rem(steps - step, steps)

    barrier = pltpu.get_barrier_semaphore()

    def greet(i, carry):
        pl.semaphore_signal(barrier, inc=1, device_id={"ep": lax.rem(me + 2 * i, devices)})
        return carry

    lax.fori_loop(1, devices // 2, greet, 0)
    pl.semaphore_signal(barrier, inc=1, device_id={"ep": twin})

    own_rows = pl.ds(pl.multiple_of(core * ff, 128), ff)
    own_weights = [
        (wg_hbm.at[0], wg.at[core]),
        (wu_hbm.at[0], wu.at[core]),
        (wd_hbm.at[0], wd.at[own_rows]),
    ]
    local_w = [
        pltpu.make_async_copy(src, dst, w_sem.at[i]) for i, (src, dst) in enumerate(own_weights)
    ]
    remote_w = [
        pltpu.make_async_remote_copy(
            src, dst, w_send.at[i], w_recv.at[i], device_id={"ep": twin}
        )
        for i, (src, dst) in enumerate(own_weights)
    ]
    for copy in local_w:
        copy.start()

    values = tokens_ref[...].astype(F32)
    scale = lax.rsqrt(jnp.mean(values * values, axis=-1, keepdims=True) + 1e-06)
    normed[...] = (values * scale * gain_ref[...].astype(F32)).astype(BF16)

    lane = iota((tok, tok), 1)
    named = [
        jnp.where(lane == routing_ref[:, k : k + 1], 1.0, 0.0).astype(F32) for k in range(2)
    ]
    earlier = jnp.where(lane < iota((tok, tok), 0), 1.0, 0.0).astype(BF16)
    before = dot(earlier, (named[0] + named[1]).astype(BF16))
    places = jnp.zeros((tok, tok), F32)
    for k in range(2):
        slot = jnp.sum(named[k] * before, axis=-1, keepdims=True)
        place = routing_ref[:, k : k + 1].astype(F32) * cap + slot
        places = jnp.where(lane == k, place, places)
        weight[:, k : k + 1] = place
    target[...] = places.T

    def block_of(expert):
        row = iota((2 * SUB, tok), 0)
        slot = jnp.where(row < SUB, row, SUB + row % extra)
        wanted = (expert * cap + slot).astype(F32)
        pick = jnp.where(target[0:1, :] == wanted, 1.0, 0.0) + jnp.where(
            target[1:2, :] == wanted, 1.0, 0.0
        )
        return dot(pick.astype(BF16), normed[...])

    def put_block(picked, ref):
        at = iota((SUB, part_w), 0) // extra
        folded = jnp.zeros((SUB, part_w), F32)
        for q in range(folds):
            columns = slice(q * part_w, (q + 1) * part_w)
            ref[q * SUB : (q + 1) * SUB, :] = picked[:SUB, columns].astype(BF16)
            folded = jnp.where(at == q, picked[SUB:, columns], folded)
        ref[folds * SUB :, :] = folded.astype(BF16)

    def send_to(expert, role_at, slot_step, slot_side):
        return pltpu.make_async_remote_copy(
            outgoing.at[expert],
            mine.at[slot_step, slot_side],
            d_send.at[expert],
            d_recv.at[slot_step * 2 + slot_side],
            device_id={"ep": device_of(expert, role_at)},
        )

    def dispatch(step):
        delta = delta_of(step)

        @pl.when(delta == 0)
        def _():
            far = lax.rem(pair + steps, experts)
            put_block(block_of(far), outgoing.at[far])
            send_to(far, 1 - role, 0, 1).start()
            put_block(block_of(pair), mine.at[0, 0])

        @pl.when(delta != 0)
        def _():
            for role_at in range(2):
                expert = lax.rem(pair + (1 - 2 * role_at) * delta + experts, experts)
                put_block(block_of(expert), outgoing.at[expert])
                send_to(expert, role_at, delta, role).start()

    def wait_arrival(slot_step, slot_side):
        pltpu.make_async_remote_copy(
            outgoing.at[0],
            mine.at[slot_step, slot_side],
            d_send.at[0],
            d_recv.at[slot_step * 2 + slot_side],
            device_id={"ep": mate},
        ).wait_recv()

    def relay(delta):
        return pltpu.make_async_remote_copy(
            mine.at[delta],
            theirs.at[delta],
            l_send.at[delta],
            l_recv.at[delta],
            device_id={"ep": mate},
        )

    def give(delta):
        return pltpu.make_async_remote_copy(
            given.at[delta],
            part.at[delta],
            p_send.at[delta],
            p_recv.at[delta],
            device_id={"ep": mate},
        )

    def send_back(delta, side):
        source = pair + (2 * role - 1) * delta
        return pltpu.make_async_remote_copy(
            final.at[delta, side],
            returned.at[pair],
            r_send.at[delta * 2 + side],
            r_recv.at[pair],
            device_id={"ep": device_of(source, side)},
        )

    def send_back_far():
        return pltpu.make_async_remote_copy(
            final.at[0, 1],
            returned.at[pair],
            r_send.at[1],
            r_recv.at[pair],
            device_id={"ep": device_of(pair + steps, 1 - role)},
        )

    def compute(delta):
        blocks = [mine.at[delta, 0], mine.at[delta, 1], theirs.at[delta, 0], theirs.at[delta, 1]]
        count = len(blocks)
        for b, block in enumerate(blocks):
            for q in range(folds):
                rows[b * SUB : (b + 1) * SUB, q * part_w : (q + 1) * part_w] = block[
                    q * SUB : (q + 1) * SUB, :
                ]
        folded = jnp.concatenate([block[folds * SUB :, :] for block in blocks], axis=0)
        main = count * SUB
        to = iota((count * extra, main), 0)
        at = iota((count * extra, main), 1)
        for q in range(folds):
            source = to // extra * SUB + q * extra + to % extra
            unfold = jnp.where(at == source, 1.0, 0.0).astype(BF16)
            rows[main:, q * part_w : (q + 1) * part_w] = dot(unfold, folded).astype(BF16)

        def half(h, carry):
            gate = dot(rows[...], wg[h])
            up = dot(rows[...], wu[h])
            hidden[h] = (jax.nn.silu(gate) * up).astype(BF16)
            return carry

        lax.fori_loop(0, 2, half, 0)
        to = iota((main, count * extra), 0)
        at = iota((main, count * extra), 1)
        refolded = jnp.zeros((main, part_w), F32)
        for q in range(folds):
            columns = slice(q * part_w, (q + 1) * part_w)
            piece = dot(hidden[0], wd[:ff, columns]) + dot(hidden[1], wd[ff:, columns])
            for b in range(2):
                kept[delta, b, q * SUB : (q + 1) * SUB, :] = piece[b * SUB : (b + 1) * SUB]
                given[delta, b, q * SUB : (q + 1) * SUB, :] = piece[
                    (b + 2) * SUB : (b + 3) * SUB
                ].astype(BF16)
            fold = (to // SUB == at // extra) & (to % SUB == q * extra + at % extra)
            refolded += dot(jnp.where(fold, 1.0, 0.0).astype(BF16), piece[main:].astype(BF16))
        for b in range(2):
            kept[delta, b, folds * SUB :, :] = refolded[b * SUB : (b + 1) * SUB]
            given[delta, b, folds * SUB :, :] = refolded[(b + 2) * SUB : (b + 3) * SUB].astype(BF16)

    pl.semaphore_wait(barrier, devices // 2)
    for step in range(WINDOW):
        dispatch(step)
    for copy in remote_w:
        copy.start()

    def body(step, carry):
        @pl.when(step < steps)
        def _():
            delta = delta_of(step)

            @pl.when(delta != 0)
            def _():
                wait_arrival(delta, 0)

            wait_arrival(delta, 1)
            relay(delta).start()

        @pl.when(step + WINDOW < steps)
        def _():
            dispatch(step + WINDOW)

        @pl.when((step >= 1) & (step <= steps))
        def _():
            delta = delta_of(step - 1)

            @pl.when(step == 1)
            def _():
                for copy in local_w:
                    copy.wait()
                for copy in remote_w:
                    copy.wait_recv()

            relay(delta).wait_recv()
            compute(delta)
            give(delta).start()

        @pl.when(step >= 2)
        def _():
            delta = delta_of(step - 2)
            give(delta).wait_recv()

            @pl.when(delta != 0)
            def _():
                final[delta] = (kept[delta] + part[delta].astype(F32)).astype(BF16)
                for side in range(2):
                    send_back(delta, side).start()

            @pl.when(delta == 0)
            def _():
                final[0, 1] = (kept[0, 1] + part[0, 1].astype(F32)).astype(BF16)
                send_back_far().start()
                returned[pair] = (kept[0, 0] + part[0, 0].astype(F32)).astype(BF16)

        return carry

    lax.fori_loop(0, steps + 2, body, 0)

    def wait_return(i, carry):
        expert = lax.rem(pair + i, experts)
        pltpu.make_async_remote_copy(
            final.at[0, 1],
            returned.at[expert],
            r_send.at[0],
            r_recv.at[expert],
            device_id={"ep": mate},
        ).wait_recv()
        return carry

    lax.fori_loop(1, experts, wait_return, 0)

    main = experts * SUB
    column = iota((tok, main), 1)
    wanted = (column // SUB * cap + column % SUB).astype(F32)
    wanted_extra = (column // SUB * cap + SUB + column % extra).astype(F32)
    share = jnp.zeros((tok, main), F32)
    share_extra = jnp.zeros((tok, main), F32)
    for k in range(2):
        place, gate = weight[:, k : k + 1], gates_ref[:, k : k + 1]
        share = jnp.where(place == wanted, gate, share)
        share_extra = jnp.where(place == wanted_extra, gate, share_extra)

    def split(value):
        high = value.astype(BF16)
        return high, (value - high.astype(F32)).astype(BF16)

    high, low = split(share)
    folded = returned[:, folds * SUB :, :].reshape(main, part_w)
    for q in range(folds):
        mask = column % SUB // extra == q
        high_extra, low_extra = split(jnp.where(mask, share_extra, 0.0))
        straight = returned[:, q * SUB : (q + 1) * SUB, :].reshape(main, part_w)
        mixed = dot(high, straight) + dot(low, straight)
        mixed += dot(high_extra, folded) + dot(low_extra, folded)
        out_ref[:, q * part_w : (q + 1) * part_w] = mixed.astype(BF16)

    for copy in remote_w:
        copy.wait_send()

    def drain(delta, carry):
        relay(delta).wait_send()
        give(delta).wait_send()

        @pl.when(delta != 0)
        def _():
            for side in range(2):
                send_back(delta, side).wait_send()

        @pl.when(delta == 0)
        def _():
            send_back_far().wait_send()

        return carry

    lax.fori_loop(0, steps, drain, 0)

    def drain_dispatch(i, carry):
        expert = lax.rem(pair + i, experts)
        send_to(expert, 0, 0, 1).wait_send()
        return carry

    lax.fori_loop(1, experts, drain_dispatch, 0)


def per_device(tokens, routing, gates, norm_gain, w_gate, w_up, w_down):
    tok, width = tokens.shape
    top = routing.shape[1]
    ff = w_gate.shape[2]
    devices = lax.axis_size("ep")
    experts = devices // GROUP
    steps = experts // 2
    cap = GROUP * (5 * tok * top // (4 * devices))
    extra = cap - SUB
    folds = SUB // extra
    assert top == 2 and 0 < extra and folds * extra == SUB and width % (folds * 128) == 0
    block = ((folds + 1) * SUB, width // folds)
    batch = 4 * cap
    pairs = (steps, 2) + block
    dma = pltpu.SemaphoreType.DMA
    vmem = pl.BlockSpec(memory_space=pltpu.VMEM)
    hbm = pl.BlockSpec(memory_space=pl.ANY)
    return pl.pallas_call(
        functools.partial(layer_kernel, devices, cap),
        out_shape=jax.ShapeDtypeStruct((tok, width), BF16),
        in_specs=[vmem, vmem, vmem, vmem, hbm, hbm, hbm],
        out_specs=vmem,
        scratch_shapes=[
            pltpu.VMEM((2, width, ff), BF16),
            pltpu.VMEM((2, width, ff), BF16),
            pltpu.VMEM((2 * ff, width), BF16),
            pltpu.VMEM((tok, width), BF16),
            pltpu.VMEM((tok, tok), F32),
            pltpu.VMEM((tok, 128), F32),
            pltpu.VMEM((experts,) + block, BF16),
            pltpu.VMEM(pairs, BF16),
            pltpu.VMEM(pairs, BF16),
            pltpu.VMEM((batch, width), BF16),
            pltpu.VMEM((2, batch, ff), BF16),
            pltpu.VMEM(pairs, F32),
            pltpu.VMEM(pairs, BF16),
            pltpu.VMEM(pairs, BF16),
            pltpu.VMEM(pairs, BF16),
            pltpu.VMEM((experts,) + block, BF16),
            dma((3,)),
            dma((3,)),
            dma((3,)),
            dma((experts,)),
            dma((experts,)),
            dma((steps,)),
            dma((steps,)),
            dma((steps,)),
            dma((steps,)),
            dma((experts,)),
            dma((experts,)),
        ],
        compiler_params=pltpu.CompilerParams(
            collective_id=0, has_side_effects=True, vmem_limit_bytes=60 * 1024 * 1024
        ),
    )(tokens, routing, gates, norm_gain.reshape(1, width), w_gate, w_up, w_down)


def solution(mesh):
    placed = (
        P(("grp", "ep"), None),
        P(("grp", "ep"), None),
        P(("grp", "ep"), None),
        P(),
        P("ep", None, None),
        P("ep", None, None),
        P("ep", None, None),
    )
    return jax.shard_map(
        per_device, mesh=mesh, in_specs=placed, out_specs=P(("grp", "ep"), None), check_vma=False
    )
```

```python
import functools

import jax
import jax.numpy as jnp
from jax import lax
from jax.experimental import pallas as pl
from jax.experimental.pallas import tpu as pltpu
from jax.sharding import PartitionSpec as P

GROUP = 4
LANES = 128
SUB = 16
F32, BF16 = jnp.float32, jnp.bfloat16


def dot(a, b):
    return jnp.dot(a, b, preferred_element_type=F32)


def iota(shape, dim):
    return lax.broadcasted_iota(jnp.int32, shape, dim)


def layer_kernel(
    devices,
    cap,
    tokens_ref,
    routing_ref,
    gates_ref,
    gain_ref,
    wg_hbm,
    wu_hbm,
    wd_hbm,
    out_ref,
    wg,
    wu,
    wd,
    normed,
    target,
    weight,
    total,
    outgoing,
    mine,
    theirs,
    rows,
    hidden,
    kept,
    given,
    part,
    final,
    returned,
    w_sem,
    w_send,
    w_recv,
    d_send,
    d_recv,
    l_send,
    l_recv,
    p_send,
    p_recv,
    r_send,
    r_recv,
):
    tok, width = tokens_ref.shape
    ff = wg_hbm.shape[2]
    extra = cap - SUB
    folds = SUB // extra
    part_w = width // folds
    experts = devices // GROUP
    steps = experts // 2

    me = lax.axis_index("ep")
    core = me % 2
    pair = me // GROUP
    role = me // 2 % 2
    mate = me + 2 - 4 * role
    twin = me + 1 - 2 * core

    def device_of(pair_at, role_at):
        return lax.rem(pair_at + 2 * experts, experts) * GROUP + role_at * 2 + core

    def delta_of(step):
        rising = lax.rem(2 * step + 2, steps)
        return jnp.where(step < steps // 2, rising, 2 * (steps - step) - 1)

    barrier = pltpu.get_barrier_semaphore()

    def greet(i, carry):
        pl.semaphore_signal(barrier, inc=1, device_id={"ep": lax.rem(me + 2 * i, devices)})
        return carry

    lax.fori_loop(1, devices // 2, greet, 0)
    pl.semaphore_signal(barrier, inc=1, device_id={"ep": twin})

    own_rows = pl.ds(pl.multiple_of(core * ff, 128), ff)
    own_weights = [
        (wg_hbm.at[0], wg.at[core]),
        (wu_hbm.at[0], wu.at[core]),
        (wd_hbm.at[0], wd.at[own_rows]),
    ]
    local_w = [
        pltpu.make_async_copy(src, dst, w_sem.at[i]) for i, (src, dst) in enumerate(own_weights)
    ]
    remote_w = [
        pltpu.make_async_remote_copy(
            src, dst, w_send.at[i], w_recv.at[i], device_id={"ep": twin}
        )
        for i, (src, dst) in enumerate(own_weights)
    ]
    for copy in local_w:
        copy.start()

    values = tokens_ref[...].astype(F32)
    scale = lax.rsqrt(jnp.mean(values * values, axis=-1, keepdims=True) + 1e-06)
    for j in range(width // LANES):
        columns = slice(j * LANES, (j + 1) * LANES)
        gain = gain_ref[j : j + 1, :].astype(F32)
        normed[:, columns] = (values[:, columns] * scale * gain).astype(BF16)

    named = [
        jnp.where(iota((experts, tok), 0) == routing_ref[k : k + 1, :], 1.0, 0.0).astype(F32)
        for k in range(2)
    ]
    earlier = jnp.where(iota((tok, tok), 0) < iota((tok, tok), 1), 1.0, 0.0).astype(BF16)
    before = dot((named[0] + named[1]).astype(BF16), earlier)
    target[...] = jnp.zeros_like(target)
    for k in range(2):
        slot = jnp.sum(named[k] * before, axis=0, keepdims=True)
        target[k : k + 1, :] = routing_ref[k : k + 1, :].astype(F32) * cap + slot

    def block_of(expert):
        row = iota((2 * SUB, tok), 0)
        slot = jnp.where(row < SUB, row, SUB + row % extra)
        wanted = (expert * cap + slot).astype(F32)
        pick = jnp.where(target[0:1, :] == wanted, 1.0, 0.0) + jnp.where(
            target[1:2, :] == wanted, 1.0, 0.0
        )
        return dot(pick.astype(BF16), normed[...])

    def put_block(picked, ref):
        at = iota((SUB, part_w), 0) // extra
        folded = jnp.zeros((SUB, part_w), F32)
        for q in range(folds):
            columns = slice(q * part_w, (q + 1) * part_w)
            ref[q * SUB : (q + 1) * SUB, :] = picked[:SUB, columns].astype(BF16)
            folded = jnp.where(at == q, picked[SUB:, columns], folded)
        ref[folds * SUB :, :] = folded.astype(BF16)

    def send_to(expert, role_at, slot_step, slot_side):
        return pltpu.make_async_remote_copy(
            outgoing.at[expert],
            mine.at[slot_step, slot_side],
            d_send.at[expert],
            d_recv.at[slot_step * 2 + slot_side],
            device_id={"ep": device_of(expert, role_at)},
        )

    def dispatch(step):
        delta = delta_of(step)

        @pl.when(delta == 0)
        def _():
            far = lax.rem(pair + steps, experts)
            put_block(block_of(far), outgoing.at[far])
            send_to(far, 1 - role, 0, 1).start()
            put_block(block_of(pair), mine.at[0, 0])

        @pl.when(delta != 0)
        def _():
            for role_at in range(2):
                expert = lax.rem(pair + (1 - 2 * role_at) * delta + experts, experts)
                put_block(block_of(expert), outgoing.at[expert])
                send_to(expert, role_at, delta, role).start()

    def wait_arrival(slot_step, slot_side):
        pltpu.make_async_remote_copy(
            outgoing.at[0],
            mine.at[slot_step, slot_side],
            d_send.at[0],
            d_recv.at[slot_step * 2 + slot_side],
            device_id={"ep": mate},
        ).wait_recv()

    def relay(delta):
        return pltpu.make_async_remote_copy(
            mine.at[delta],
            theirs.at[delta],
            l_send.at[delta],
            l_recv.at[delta],
            device_id={"ep": mate},
        )

    def give(delta):
        return pltpu.make_async_remote_copy(
            given.at[delta],
            part.at[delta],
            p_send.at[delta],
            p_recv.at[delta],
            device_id={"ep": mate},
        )

    def send_back(delta, side):
        source = pair + (2 * role - 1) * delta
        return pltpu.make_async_remote_copy(
            final.at[delta, side],
            returned.at[pair],
            r_send.at[delta * 2 + side],
            r_recv.at[pair],
            device_id={"ep": device_of(source, side)},
        )

    def send_back_far():
        return pltpu.make_async_remote_copy(
            final.at[0, 1],
            returned.at[pair],
            r_send.at[1],
            r_recv.at[pair],
            device_id={"ep": device_of(pair + steps, 1 - role)},
        )

    def compute(delta):
        blocks = [mine.at[delta, 0], mine.at[delta, 1], theirs.at[delta, 0], theirs.at[delta, 1]]
        count = len(blocks)
        for b, block in enumerate(blocks):
            for q in range(folds):
                rows[b * SUB : (b + 1) * SUB, q * part_w : (q + 1) * part_w] = block[
                    q * SUB : (q + 1) * SUB, :
                ]
        folded = jnp.concatenate([block[folds * SUB :, :] for block in blocks], axis=0)
        main = count * SUB
        to = iota((count * extra, main), 0)
        at = iota((count * extra, main), 1)
        for q in range(folds):
            source = to // extra * SUB + q * extra + to % extra
            unfold = jnp.where(at == source, 1.0, 0.0).astype(BF16)
            rows[main:, q * part_w : (q + 1) * part_w] = dot(unfold, folded).astype(BF16)

        def half(h, carry):
            gate = dot(rows[...], wg[h])
            up = dot(rows[...], wu[h])
            hidden[h] = (jax.nn.silu(gate) * up).astype(BF16)
            return carry

        lax.fori_loop(0, 2, half, 0)
        to = iota((main, count * extra), 0)
        at = iota((main, count * extra), 1)
        refolded = jnp.zeros((main, part_w), F32)
        for q in range(folds):
            columns = slice(q * part_w, (q + 1) * part_w)
            piece = dot(hidden[0], wd[:ff, columns]) + dot(hidden[1], wd[ff:, columns])
            for b in range(2):
                kept[delta, b, q * SUB : (q + 1) * SUB, :] = piece[b * SUB : (b + 1) * SUB]
                given[delta, b, q * SUB : (q + 1) * SUB, :] = piece[
                    (b + 2) * SUB : (b + 3) * SUB
                ].astype(BF16)
            fold = (to // SUB == at // extra) & (to % SUB == q * extra + at % extra)
            refolded += dot(jnp.where(fold, 1.0, 0.0).astype(BF16), piece[main:].astype(BF16))
        for b in range(2):
            kept[delta, b, folds * SUB :, :] = refolded[b * SUB : (b + 1) * SUB]
            given[delta, b, folds * SUB :, :] = refolded[(b + 2) * SUB : (b + 3) * SUB].astype(BF16)

    pl.semaphore_wait(barrier, devices // 2)

    def dispatch_all(step, carry):
        dispatch(step)

        @pl.when(step == 1)
        def _():
            for copy in remote_w:
                copy.start()

        return carry

    lax.fori_loop(0, steps, dispatch_all, 0)

    def body(step, carry):
        @pl.when(step < steps)
        def _():
            delta = delta_of(step)

            @pl.when(delta != 0)
            def _():
                wait_arrival(delta, 0)

            wait_arrival(delta, 1)
            relay(delta).start()

        @pl.when((step >= 1) & (step <= steps))
        def _():
            delta = delta_of(step - 1)

            @pl.when(step == 1)
            def _():
                for copy in local_w:
                    copy.wait()
                for copy in remote_w:
                    copy.wait_recv()

            relay(delta).wait_recv()
            compute(delta)
            give(delta).start()

        @pl.when(step >= 2)
        def _():
            delta = delta_of(step - 2)
            give(delta).wait_recv()

            @pl.when(delta != 0)
            def _():
                final[delta] = (kept[delta] + part[delta].astype(F32)).astype(BF16)
                for side in range(2):
                    send_back(delta, side).start()

            @pl.when(delta == 0)
            def _():
                final[0, 1] = (kept[0, 1] + part[0, 1].astype(F32)).astype(BF16)
                send_back_far().start()
                returned[pair] = (kept[0, 0] + part[0, 0].astype(F32)).astype(BF16)

        return carry

    lax.fori_loop(0, steps + 2, body, 0)

    target[2:4, :] = gates_ref[...]
    weight[...] = target[...].T
    total[...] = jnp.zeros_like(total)

    def wait_return(expert):
        pltpu.make_async_remote_copy(
            final.at[0, 1],
            returned.at[expert],
            r_send.at[0],
            r_recv.at[expert],
            device_id={"ep": mate},
        ).wait_recv()

    def split(value):
        high = value.astype(BF16)
        return [high, (value - high.astype(F32)).astype(BF16)]

    def collect(i, carry):
        near = [delta_of(2 * i), delta_of(2 * i + 1)]
        group = []
        for delta in near:
            group.append(lax.rem(pair + jnp.where(delta == 0, steps, delta), experts))
            group.append(lax.rem(pair - delta + experts, experts))
        count = len(group) * SUB
        column = iota((tok, count), 1)
        row = column % SUB
        first = jnp.zeros((tok, count), jnp.int32)
        for j, expert in enumerate(group):
            first = jnp.where(column // SUB == j, expert * cap, first)
        straight = jnp.zeros((tok, count), F32)
        folded = jnp.zeros((tok, count), F32)
        for k in range(2):
            place, gate = weight[:, k : k + 1], weight[:, k + 2 : k + 3]
            straight = jnp.where(place == (first + row).astype(F32), gate, straight)
            folded = jnp.where(place == (first + SUB + row % extra).astype(F32), gate, folded)
        shares = jnp.concatenate(split(straight), axis=0)
        shares_folded = []
        for q in range(folds):
            shares_folded += split(jnp.where(row // extra == q, folded, 0.0))
        shares_folded = jnp.concatenate(shares_folded, axis=0)

        for j, (delta, expert) in enumerate(zip([near[0], near[0], near[1], near[1]], group)):
            if j % 2 == 0:
                wait_return(expert)
            else:

                @pl.when(delta != 0)
                def _():
                    wait_return(expert)

        def rows_of(q):
            return jnp.concatenate(
                [returned[expert, q * SUB : (q + 1) * SUB, :] for expert in group], axis=0
            )

        more = dot(shares_folded, rows_of(folds))
        for q in range(folds):
            some = dot(shares, rows_of(q))
            part_sum = some[:tok] + some[tok:]
            part_sum += more[2 * q * tok : (2 * q + 1) * tok]
            part_sum += more[(2 * q + 1) * tok : (2 * q + 2) * tok]
            total[:, q * part_w : (q + 1) * part_w] += part_sum
        return carry

    lax.fori_loop(0, steps // 2, collect, 0)
    out_ref[...] = total[...].astype(BF16)

    for copy in remote_w:
        copy.wait_send()

    def drain(delta, carry):
        relay(delta).wait_send()
        give(delta).wait_send()

        @pl.when(delta != 0)
        def _():
            for side in range(2):
                send_back(delta, side).wait_send()

        @pl.when(delta == 0)
        def _():
            send_back_far().wait_send()

        return carry

    lax.fori_loop(0, steps, drain, 0)

    def drain_dispatch(i, carry):
        expert = lax.rem(pair + i, experts)
        send_to(expert, 0, 0, 1).wait_send()
        return carry

    lax.fori_loop(1, experts, drain_dispatch, 0)


def per_device(tokens, routing, gates, norm_gain, w_gate, w_up, w_down):
    tok, width = tokens.shape
    top = routing.shape[1]
    ff = w_gate.shape[2]
    devices = lax.axis_size("ep")
    experts = devices // GROUP
    steps = experts // 2
    cap = GROUP * (5 * tok * top // (4 * devices))
    extra = cap - SUB
    folds = SUB // extra
    assert top == 2 and tok == LANES and steps % 2 == 0
    assert 0 < extra and folds * extra == SUB and width % (folds * LANES) == 0
    block = ((folds + 1) * SUB, width // folds)
    batch = 4 * cap
    pairs = (steps, 2) + block
    dma = pltpu.SemaphoreType.DMA
    vmem = pl.BlockSpec(memory_space=pltpu.VMEM)
    hbm = pl.BlockSpec(memory_space=pl.ANY)
    return pl.pallas_call(
        functools.partial(layer_kernel, devices, cap),
        out_shape=jax.ShapeDtypeStruct((tok, width), BF16),
        in_specs=[vmem, vmem, vmem, vmem, hbm, hbm, hbm],
        out_specs=vmem,
        scratch_shapes=[
            pltpu.VMEM((2, width, ff), BF16),
            pltpu.VMEM((2, width, ff), BF16),
            pltpu.VMEM((2 * ff, width), BF16),
            pltpu.VMEM((tok, width), BF16),
            pltpu.VMEM((tok, tok), F32),
            pltpu.VMEM((tok, tok), F32),
            pltpu.VMEM((tok, width), F32),
            pltpu.VMEM((experts,) + block, BF16),
            pltpu.VMEM(pairs, BF16),
            pltpu.VMEM(pairs, BF16),
            pltpu.VMEM((batch, width), BF16),
            pltpu.VMEM((2, batch, ff), BF16),
            pltpu.VMEM(pairs, F32),
            pltpu.VMEM(pairs, BF16),
            pltpu.VMEM(pairs, BF16),
            pltpu.VMEM(pairs, BF16),
            pltpu.VMEM((experts,) + block, BF16),
            dma((3,)),
            dma((3,)),
            dma((3,)),
            dma((experts,)),
            dma((experts,)),
            dma((steps,)),
            dma((steps,)),
            dma((steps,)),
            dma((steps,)),
            dma((experts,)),
            dma((experts,)),
        ],
        compiler_params=pltpu.CompilerParams(
            collective_id=0, has_side_effects=True, vmem_limit_bytes=60 * 1024 * 1024
        ),
    )(tokens, routing.T, gates.T, norm_gain.reshape(width // LANES, LANES), w_gate, w_up, w_down)


def solution(mesh):
    placed = (
        P(("grp", "ep"), None),
        P(("grp", "ep"), None),
        P(("grp", "ep"), None),
        P(),
        P("ep", None, None),
        P("ep", None, None),
        P("ep", None, None),
    )
    return jax.shard_map(
        per_device, mesh=mesh, in_specs=placed, out_specs=P(("grp", "ep"), None), check_vma=False
    )
```

```python
import functools

import jax
import jax.numpy as jnp
from jax import lax
from jax.experimental import pallas as pl
from jax.experimental.pallas import tpu as pltpu
from jax.sharding import PartitionSpec as P

GROUP = 4
LANES = 128
WINDOW = 4
SUB = 16
F32, BF16 = jnp.float32, jnp.bfloat16


def dot(a, b):
    return jnp.dot(a, b, preferred_element_type=F32)


def iota(shape, dim):
    return lax.broadcasted_iota(jnp.int32, shape, dim)


def layer_kernel(
    devices,
    cap,
    tokens_hbm,
    routing_ref,
    gates_ref,
    gain_ref,
    wg_hbm,
    wu_hbm,
    wd_hbm,
    out_ref,
    wg,
    wu,
    wd,
    tokens_ref,
    normed,
    target,
    weight,
    total,
    outgoing,
    mine,
    theirs,
    rows,
    hidden,
    kept,
    given,
    part,
    final,
    returned,
    up,
    down,
    t_sem,
    w_sem,
    w_send,
    w_recv,
    d_send,
    d_recv,
    l_send,
    l_recv,
    p_send,
    p_recv,
    r_send,
    r_recv,
):
    tok, width = tokens_hbm.shape
    ff = wg_hbm.shape[2]
    extra = cap - SUB
    folds = SUB // extra
    part_w = width // folds
    experts = devices // GROUP
    steps = experts // 2

    me = lax.axis_index("ep")
    core = me % 2
    pair = me // GROUP
    role = me // 2 % 2
    mate = me + 2 - 4 * role
    twin = me + 1 - 2 * core

    def device_of(pair_at, role_at):
        return lax.rem(pair_at + 2 * experts, experts) * GROUP + role_at * 2 + core

    def delta_of(step):
        rising = lax.rem(2 * step + 2, steps)
        return jnp.where(step < steps // 2, rising, 2 * (steps - step) - 1)

    below, above = lax.rem(me + devices - 2, devices), lax.rem(me + 2, devices)
    reach = devices // 4 - 1
    barrier = pltpu.get_barrier_semaphore()
    for other in (below, above, twin):
        pl.semaphore_signal(barrier, inc=1, device_id={"ep": other})

    def pass_on(k):
        pl.semaphore_signal(up.at[k], inc=1, device_id={"ep": below})
        pl.semaphore_signal(down.at[k], inc=1, device_id={"ep": above})

    def learn(k, carry):
        pl.semaphore_wait(up.at[k], 1)
        pl.semaphore_wait(down.at[k], 1)

        @pl.when(k + 1 < reach)
        def _():
            pass_on(k + 1)

        return carry

    fetch = pltpu.make_async_copy(tokens_hbm, tokens_ref, t_sem)
    fetch.start()
    own_rows = pl.ds(pl.multiple_of(core * ff, 128), ff)
    own_weights = [
        (wg_hbm.at[0], wg.at[core]),
        (wu_hbm.at[0], wu.at[core]),
        (wd_hbm.at[0], wd.at[own_rows]),
    ]
    local_w = [
        pltpu.make_async_copy(src, dst, w_sem.at[i]) for i, (src, dst) in enumerate(own_weights)
    ]
    remote_w = [
        pltpu.make_async_remote_copy(
            src, dst, w_send.at[i], w_recv.at[i], device_id={"ep": twin}
        )
        for i, (src, dst) in enumerate(own_weights)
    ]
    for copy in local_w:
        copy.start()

    named = [
        jnp.where(iota((experts, tok), 0) == routing_ref[k : k + 1, :], 1.0, 0.0).astype(F32)
        for k in range(2)
    ]
    earlier = jnp.where(iota((tok, tok), 0) < iota((tok, tok), 1), 1.0, 0.0).astype(BF16)
    before = dot((named[0] + named[1]).astype(BF16), earlier)
    target[...] = jnp.zeros_like(target)
    for k in range(2):
        slot = jnp.sum(named[k] * before, axis=0, keepdims=True)
        target[k : k + 1, :] = routing_ref[k : k + 1, :].astype(F32) * cap + slot

    fetch.wait()
    values = tokens_ref[...].astype(F32)
    scale = lax.rsqrt(jnp.mean(values * values, axis=-1, keepdims=True) + 1e-06)
    for j in range(width // LANES):
        columns = slice(j * LANES, (j + 1) * LANES)
        gain = gain_ref[j : j + 1, :].astype(F32)
        normed[:, columns] = (values[:, columns] * scale * gain).astype(BF16)

    def block_of(expert):
        row = iota((2 * SUB, tok), 0)
        slot = jnp.where(row < SUB, row, SUB + row % extra)
        wanted = (expert * cap + slot).astype(F32)
        pick = jnp.where(target[0:1, :] == wanted, 1.0, 0.0) + jnp.where(
            target[1:2, :] == wanted, 1.0, 0.0
        )
        return dot(pick.astype(BF16), normed[...])

    def put_block(picked, ref):
        at = iota((SUB, part_w), 0) // extra
        folded = jnp.zeros((SUB, part_w), F32)
        for q in range(folds):
            columns = slice(q * part_w, (q + 1) * part_w)
            ref[q * SUB : (q + 1) * SUB, :] = picked[:SUB, columns].astype(BF16)
            folded = jnp.where(at == q, picked[SUB:, columns], folded)
        ref[folds * SUB :, :] = folded.astype(BF16)

    def send_to(expert, role_at, slot_step, slot_side):
        return pltpu.make_async_remote_copy(
            outgoing.at[expert],
            mine.at[slot_step, slot_side],
            d_send.at[expert],
            d_recv.at[slot_step * 2 + slot_side],
            device_id={"ep": device_of(expert, role_at)},
        )

    def dispatch(step):
        delta = delta_of(step)
        known = jnp.maximum(4 * step, 1)
        wanted = jnp.where(step < steps // 2, jnp.minimum(4 * step + 4, reach), known)
        lax.fori_loop(known, wanted, learn, 0)

        @pl.when(delta == 0)
        def _():
            far = lax.rem(pair + steps, experts)
            put_block(block_of(far), outgoing.at[far])
            send_to(far, 1 - role, 0, 1).start()
            put_block(block_of(pair), mine.at[0, 0])

        @pl.when(delta != 0)
        def _():
            for role_at in range(2):
                expert = lax.rem(pair + (1 - 2 * role_at) * delta + experts, experts)
                put_block(block_of(expert), outgoing.at[expert])
                send_to(expert, role_at, delta, role).start()

    def wait_arrival(slot_step, slot_side):
        pltpu.make_async_remote_copy(
            outgoing.at[0],
            mine.at[slot_step, slot_side],
            d_send.at[0],
            d_recv.at[slot_step * 2 + slot_side],
            device_id={"ep": mate},
        ).wait_recv()

    def relay(delta, side):
        return pltpu.make_async_remote_copy(
            mine.at[delta, side],
            theirs.at[delta, side],
            l_send.at[2 * delta + side],
            l_recv.at[2 * delta + side],
            device_id={"ep": mate},
        )

    def give(delta):
        return pltpu.make_async_remote_copy(
            given.at[delta],
            part.at[delta],
            p_send.at[delta],
            p_recv.at[delta],
            device_id={"ep": mate},
        )

    def send_back(delta, side):
        source = pair + (2 * role - 1) * delta
        return pltpu.make_async_remote_copy(
            final.at[delta, side],
            returned.at[pair],
            r_send.at[delta * 2 + side],
            r_recv.at[pair],
            device_id={"ep": device_of(source, side)},
        )

    def send_back_far():
        return pltpu.make_async_remote_copy(
            final.at[0, 1],
            returned.at[pair],
            r_send.at[1],
            r_recv.at[pair],
            device_id={"ep": device_of(pair + steps, 1 - role)},
        )

    def compute(delta):
        blocks = [mine.at[delta, 0], mine.at[delta, 1], theirs.at[delta, 0], theirs.at[delta, 1]]
        count = len(blocks)
        for b, block in enumerate(blocks):
            for q in range(folds):
                rows[b * SUB : (b + 1) * SUB, q * part_w : (q + 1) * part_w] = block[
                    q * SUB : (q + 1) * SUB, :
                ]
        folded = jnp.concatenate([block[folds * SUB :, :] for block in blocks], axis=0)
        main = count * SUB
        to = iota((count * extra, main), 0)
        at = iota((count * extra, main), 1)
        for q in range(folds):
            source = to // extra * SUB + q * extra + to % extra
            unfold = jnp.where(at == source, 1.0, 0.0).astype(BF16)
            rows[main:, q * part_w : (q + 1) * part_w] = dot(unfold, folded).astype(BF16)

        def half(h, carry):
            gate = dot(rows[...], wg[h])
            up = dot(rows[...], wu[h])
            hidden[h] = (jax.nn.silu(gate) * up).astype(BF16)
            return carry

        lax.fori_loop(0, 2, half, 0)
        to = iota((main, count * extra), 0)
        at = iota((main, count * extra), 1)
        refolded = jnp.zeros((main, part_w), F32)
        for q in range(folds):
            columns = slice(q * part_w, (q + 1) * part_w)
            piece = dot(hidden[0], wd[:ff, columns]) + dot(hidden[1], wd[ff:, columns])
            for b in range(2):
                kept[delta, b, q * SUB : (q + 1) * SUB, :] = piece[b * SUB : (b + 1) * SUB]
                given[delta, b, q * SUB : (q + 1) * SUB, :] = piece[
                    (b + 2) * SUB : (b + 3) * SUB
                ].astype(BF16)
            fold = (to // SUB == at // extra) & (to % SUB == q * extra + at % extra)
            refolded += dot(jnp.where(fold, 1.0, 0.0).astype(BF16), piece[main:].astype(BF16))
        for b in range(2):
            kept[delta, b, folds * SUB :, :] = refolded[b * SUB : (b + 1) * SUB]
            given[delta, b, folds * SUB :, :] = refolded[(b + 2) * SUB : (b + 3) * SUB].astype(BF16)

    pl.semaphore_wait(barrier, 3)
    pass_on(1)
    lax.fori_loop(0, WINDOW, lambda step, carry: (dispatch(step), carry)[1], 0)
    for copy in remote_w:
        copy.start()

    def body(step, carry):
        @pl.when(step < steps)
        def _():
            delta = delta_of(step)

            @pl.when(delta != 0)
            def _():
                wait_arrival(delta, 0)

            relay(delta, 0).start()
            wait_arrival(delta, 1)
            relay(delta, 1).start()

        @pl.when(step + WINDOW < steps)
        def _():
            dispatch(step + WINDOW)

        @pl.when((step >= 1) & (step <= steps))
        def _():
            delta = delta_of(step - 1)

            @pl.when(step == 1)
            def _():
                for copy in local_w:
                    copy.wait()
                for copy in remote_w:
                    copy.wait_recv()

            for side in range(2):
                relay(delta, side).wait_recv()
            compute(delta)
            give(delta).start()

        @pl.when(step >= 2)
        def _():
            delta = delta_of(step - 2)
            give(delta).wait_recv()

            @pl.when(delta != 0)
            def _():
                final[delta] = (kept[delta] + part[delta].astype(F32)).astype(BF16)
                for side in range(2):
                    send_back(delta, side).start()

            @pl.when(delta == 0)
            def _():
                final[0, 1] = (kept[0, 1] + part[0, 1].astype(F32)).astype(BF16)
                send_back_far().start()
                returned[pair] = (kept[0, 0] + part[0, 0].astype(F32)).astype(BF16)

        return carry

    lax.fori_loop(0, steps + 2, body, 0)

    target[2:4, :] = gates_ref[...]
    weight[...] = target[...].T
    total[...] = jnp.zeros_like(total)

    def wait_return(expert):
        pltpu.make_async_remote_copy(
            final.at[0, 1],
            returned.at[expert],
            r_send.at[0],
            r_recv.at[expert],
            device_id={"ep": mate},
        ).wait_recv()

    def split(value):
        high = value.astype(BF16)
        return [high, (value - high.astype(F32)).astype(BF16)]

    def collect(i, carry):
        near = [delta_of(2 * i), delta_of(2 * i + 1)]
        group = []
        for delta in near:
            group.append(lax.rem(pair + jnp.where(delta == 0, steps, delta), experts))
            group.append(lax.rem(pair - delta + experts, experts))
        count = len(group) * SUB
        column = iota((tok, count), 1)
        row = column % SUB
        first = jnp.zeros((tok, count), jnp.int32)
        for j, expert in enumerate(group):
            first = jnp.where(column // SUB == j, expert * cap, first)
        straight = jnp.zeros((tok, count), F32)
        folded = jnp.zeros((tok, count), F32)
        for k in range(2):
            place, gate = weight[:, k : k + 1], weight[:, k + 2 : k + 3]
            straight = jnp.where(place == (first + row).astype(F32), gate, straight)
            folded = jnp.where(place == (first + SUB + row % extra).astype(F32), gate, folded)
        shares = jnp.concatenate(split(straight), axis=0)
        shares_folded = []
        for q in range(folds):
            shares_folded += split(jnp.where(row // extra == q, folded, 0.0))
        shares_folded = jnp.concatenate(shares_folded, axis=0)

        for j, (delta, expert) in enumerate(zip([near[0], near[0], near[1], near[1]], group)):
            if j % 2 == 0:
                wait_return(expert)
            else:

                @pl.when(delta != 0)
                def _():
                    wait_return(expert)

        def rows_of(q):
            return jnp.concatenate(
                [returned[expert, q * SUB : (q + 1) * SUB, :] for expert in group], axis=0
            )

        more = dot(shares_folded, rows_of(folds))
        for q in range(folds):
            some = dot(shares, rows_of(q))
            part_sum = some[:tok] + some[tok:]
            part_sum += more[2 * q * tok : (2 * q + 1) * tok]
            part_sum += more[(2 * q + 1) * tok : (2 * q + 2) * tok]
            total[:, q * part_w : (q + 1) * part_w] += part_sum
        return carry

    lax.fori_loop(0, steps // 2, collect, 0)
    out_ref[...] = total[...].astype(BF16)

    for copy in remote_w:
        copy.wait_send()

    def drain(delta, carry):
        for side in range(2):
            relay(delta, side).wait_send()
        give(delta).wait_send()

        @pl.when(delta != 0)
        def _():
            for side in range(2):
                send_back(delta, side).wait_send()

        @pl.when(delta == 0)
        def _():
            send_back_far().wait_send()

        return carry

    lax.fori_loop(0, steps, drain, 0)

    def drain_dispatch(i, carry):
        expert = lax.rem(pair + i, experts)
        send_to(expert, 0, 0, 1).wait_send()
        return carry

    lax.fori_loop(1, experts, drain_dispatch, 0)


def per_device(tokens, routing, gates, norm_gain, w_gate, w_up, w_down):
    tok, width = tokens.shape
    top = routing.shape[1]
    ff = w_gate.shape[2]
    devices = lax.axis_size("ep")
    experts = devices // GROUP
    steps = experts // 2
    cap = GROUP * (5 * tok * top // (4 * devices))
    extra = cap - SUB
    folds = SUB // extra
    assert top == 2 and tok == LANES and steps % 2 == 0
    assert 0 < extra and folds * extra == SUB and width % (folds * LANES) == 0
    block = ((folds + 1) * SUB, width // folds)
    batch = 4 * cap
    pairs = (steps, 2) + block
    dma = pltpu.SemaphoreType.DMA
    vmem = pl.BlockSpec(memory_space=pltpu.VMEM)
    hbm = pl.BlockSpec(memory_space=pltpu.HBM)
    return pl.pallas_call(
        functools.partial(layer_kernel, devices, cap),
        out_shape=jax.ShapeDtypeStruct((tok, width), BF16),
        in_specs=[hbm, vmem, vmem, vmem, hbm, hbm, hbm],
        out_specs=vmem,
        scratch_shapes=[
            pltpu.VMEM((2, width, ff), BF16),
            pltpu.VMEM((2, width, ff), BF16),
            pltpu.VMEM((2 * ff, width), BF16),
            pltpu.VMEM((tok, width), BF16),
            pltpu.VMEM((tok, width), BF16),
            pltpu.VMEM((tok, tok), F32),
            pltpu.VMEM((tok, tok), F32),
            pltpu.VMEM((tok, width), F32),
            pltpu.VMEM((experts,) + block, BF16),
            pltpu.VMEM(pairs, BF16),
            pltpu.VMEM(pairs, BF16),
            pltpu.VMEM((batch, width), BF16),
            pltpu.VMEM((2, batch, ff), BF16),
            pltpu.VMEM(pairs, F32),
            pltpu.VMEM(pairs, BF16),
            pltpu.VMEM(pairs, BF16),
            pltpu.VMEM(pairs, BF16),
            pltpu.VMEM((experts,) + block, BF16),
            pltpu.SemaphoreType.REGULAR((devices // 4,)),
            pltpu.SemaphoreType.REGULAR((devices // 4,)),
            dma,
            dma((3,)),
            dma((3,)),
            dma((3,)),
            dma((experts,)),
            dma((experts,)),
            dma((experts,)),
            dma((experts,)),
            dma((steps,)),
            dma((steps,)),
            dma((experts,)),
            dma((experts,)),
        ],
        compiler_params=pltpu.CompilerParams(
            collective_id=0, has_side_effects=True, vmem_limit_bytes=60 * 1024 * 1024
        ),
    )(tokens, routing.T, gates.T, norm_gain.reshape(width // LANES, LANES), w_gate, w_up, w_down)


def solution(mesh):
    placed = (
        P(("grp", "ep"), None),
        P(("grp", "ep"), None),
        P(("grp", "ep"), None),
        P(),
        P("ep", None, None),
        P("ep", None, None),
        P("ep", None, None),
    )
    return jax.shard_map(
        per_device, mesh=mesh, in_specs=placed, out_specs=P(("grp", "ep"), None), check_vma=False
    )
```

```python
import functools

import jax
import jax.numpy as jnp
from jax import lax
from jax.experimental import pallas as pl
from jax.experimental.pallas import tpu as pltpu
from jax.sharding import PartitionSpec as P

GROUP = 4
LANES = 128
WINDOW = 8
SUB = 16
F32, BF16 = jnp.float32, jnp.bfloat16


def dot(a, b):
    return jnp.dot(a, b, preferred_element_type=F32)


def iota(shape, dim):
    return lax.broadcasted_iota(jnp.int32, shape, dim)


def layer_kernel(
    devices,
    cap,
    tokens_hbm,
    routing_ref,
    gates_ref,
    gain_ref,
    wg_hbm,
    wu_hbm,
    wd_hbm,
    out_ref,
    wg,
    wu,
    wd,
    tokens_ref,
    normed,
    target,
    weight,
    total,
    outgoing,
    mine,
    theirs,
    rows,
    hidden,
    kept,
    given,
    part,
    final,
    returned,
    up,
    down,
    t_sem,
    w_sem,
    w_send,
    w_recv,
    d_send,
    d_recv,
    l_send,
    l_recv,
    p_send,
    p_recv,
    r_send,
    r_recv,
):
    tok, width = tokens_hbm.shape
    ff = wg_hbm.shape[2]
    extra = cap - SUB
    folds = SUB // extra
    part_w = width // folds
    experts = devices // GROUP
    steps = experts // 2

    me = lax.axis_index("ep")
    core = me % 2
    pair = me // GROUP
    role = me // 2 % 2
    mate = me + 2 - 4 * role
    twin = me + 1 - 2 * core

    def device_of(pair_at, role_at):
        return lax.rem(pair_at + 2 * experts, experts) * GROUP + role_at * 2 + core

    def delta_of(step):
        rising = lax.rem(2 * step + 2, steps)
        return jnp.where(step < steps // 2, rising, 2 * (steps - step) - 1)

    below, above = lax.rem(me + devices - 2, devices), lax.rem(me + 2, devices)
    reach = devices // 4 - 1
    barrier = pltpu.get_barrier_semaphore()
    for other in (below, above, twin):
        pl.semaphore_signal(barrier, inc=1, device_id={"ep": other})

    def pass_on(k):
        pl.semaphore_signal(up.at[k], inc=1, device_id={"ep": below})
        pl.semaphore_signal(down.at[k], inc=1, device_id={"ep": above})

    def learn(k, carry):
        pl.semaphore_wait(up.at[k], 1)
        pl.semaphore_wait(down.at[k], 1)

        @pl.when(k + 1 < reach)
        def _():
            pass_on(k + 1)

        return carry

    fetch = pltpu.make_async_copy(tokens_hbm, tokens_ref, t_sem)
    fetch.start()
    own_rows = pl.ds(pl.multiple_of(core * ff, 128), ff)
    own_weights = [
        (wg_hbm.at[0], wg.at[core]),
        (wu_hbm.at[0], wu.at[core]),
        (wd_hbm.at[0], wd.at[own_rows]),
    ]
    local_w = [
        pltpu.make_async_copy(src, dst, w_sem.at[i]) for i, (src, dst) in enumerate(own_weights)
    ]
    remote_w = [
        pltpu.make_async_remote_copy(
            src, dst, w_send.at[i], w_recv.at[i], device_id={"ep": twin}
        )
        for i, (src, dst) in enumerate(own_weights)
    ]
    for copy in local_w:
        copy.start()

    named = [
        jnp.where(iota((experts, tok), 0) == routing_ref[k : k + 1, :], 1.0, 0.0).astype(F32)
        for k in range(2)
    ]
    earlier = jnp.where(iota((tok, tok), 0) < iota((tok, tok), 1), 1.0, 0.0).astype(BF16)
    before = dot((named[0] + named[1]).astype(BF16), earlier)
    target[...] = jnp.zeros_like(target)
    for k in range(2):
        slot = jnp.sum(named[k] * before, axis=0, keepdims=True)
        target[k : k + 1, :] = routing_ref[k : k + 1, :].astype(F32) * cap + slot

    fetch.wait()
    values = tokens_ref[...].astype(F32)
    scale = lax.rsqrt(jnp.mean(values * values, axis=-1, keepdims=True) + 1e-06)
    for j in range(width // LANES):
        columns = slice(j * LANES, (j + 1) * LANES)
        gain = gain_ref[j : j + 1, :].astype(F32)
        normed[:, columns] = (values[:, columns] * scale * gain).astype(BF16)

    def block_of(expert):
        row = iota((2 * SUB, tok), 0)
        slot = jnp.where(row < SUB, row, SUB + row % extra)
        wanted = (expert * cap + slot).astype(F32)
        pick = jnp.where(target[0:1, :] == wanted, 1.0, 0.0) + jnp.where(
            target[1:2, :] == wanted, 1.0, 0.0
        )
        return dot(pick.astype(BF16), normed[...])

    def put_block(picked, ref):
        at = iota((SUB, part_w), 0) // extra
        folded = jnp.zeros((SUB, part_w), F32)
        for q in range(folds):
            columns = slice(q * part_w, (q + 1) * part_w)
            ref[q * SUB : (q + 1) * SUB, :] = picked[:SUB, columns].astype(BF16)
            folded = jnp.where(at == q, picked[SUB:, columns], folded)
        ref[folds * SUB :, :] = folded.astype(BF16)

    def send_to(expert, role_at, slot_step, slot_side):
        return pltpu.make_async_remote_copy(
            outgoing.at[expert],
            mine.at[slot_step, slot_side],
            d_send.at[expert],
            d_recv.at[slot_step * 2 + slot_side],
            device_id={"ep": device_of(expert, role_at)},
        )

    def dispatch(step):
        delta = delta_of(step)
        known = jnp.maximum(4 * step, 1)
        wanted = jnp.where(step < steps // 2, jnp.minimum(4 * step + 4, reach), known)
        lax.fori_loop(known, wanted, learn, 0)

        @pl.when(delta == 0)
        def _():
            far = lax.rem(pair + steps, experts)
            put_block(block_of(far), outgoing.at[far])
            send_to(far, 1 - role, 0, 1).start()
            put_block(block_of(pair), mine.at[0, 0])

        @pl.when(delta != 0)
        def _():
            for role_at in range(2):
                expert = lax.rem(pair + (1 - 2 * role_at) * delta + experts, experts)
                put_block(block_of(expert), outgoing.at[expert])
                send_to(expert, role_at, delta, role).start()

    def wait_arrival(slot_step, slot_side):
        pltpu.make_async_remote_copy(
            outgoing.at[0],
            mine.at[slot_step, slot_side],
            d_send.at[0],
            d_recv.at[slot_step * 2 + slot_side],
            device_id={"ep": mate},
        ).wait_recv()

    def relay(delta, side):
        return pltpu.make_async_remote_copy(
            mine.at[delta, side],
            theirs.at[delta, side],
            l_send.at[2 * delta + side],
            l_recv.at[2 * delta + side],
            device_id={"ep": mate},
        )

    def give(delta):
        return pltpu.make_async_remote_copy(
            given.at[delta],
            part.at[delta],
            p_send.at[delta],
            p_recv.at[delta],
            device_id={"ep": mate},
        )

    def send_back(delta, side):
        source = pair + (2 * role - 1) * delta
        return pltpu.make_async_remote_copy(
            final.at[delta, side],
            returned.at[pair],
            r_send.at[delta * 2 + side],
            r_recv.at[pair],
            device_id={"ep": device_of(source, side)},
        )

    def send_back_far():
        return pltpu.make_async_remote_copy(
            final.at[0, 1],
            returned.at[pair],
            r_send.at[1],
            r_recv.at[pair],
            device_id={"ep": device_of(pair + steps, 1 - role)},
        )

    def compute(delta):
        blocks = [mine.at[delta, 0], mine.at[delta, 1], theirs.at[delta, 0], theirs.at[delta, 1]]
        count = len(blocks)
        for b, block in enumerate(blocks):
            for q in range(folds):
                rows[b * SUB : (b + 1) * SUB, q * part_w : (q + 1) * part_w] = block[
                    q * SUB : (q + 1) * SUB, :
                ]
        folded = jnp.concatenate([block[folds * SUB :, :] for block in blocks], axis=0)
        main = count * SUB
        to = iota((count * extra, main), 0)
        at = iota((count * extra, main), 1)
        for q in range(folds):
            source = to // extra * SUB + q * extra + to % extra
            unfold = jnp.where(at == source, 1.0, 0.0).astype(BF16)
            rows[main:, q * part_w : (q + 1) * part_w] = dot(unfold, folded).astype(BF16)

        def half(h, carry):
            gate = dot(rows[...], wg[h])
            up = dot(rows[...], wu[h])
            hidden[h] = (jax.nn.silu(gate) * up).astype(BF16)
            return carry

        lax.fori_loop(0, 2, half, 0)
        to = iota((main, count * extra), 0)
        at = iota((main, count * extra), 1)
        refolded = jnp.zeros((main, part_w), F32)
        for q in range(folds):
            columns = slice(q * part_w, (q + 1) * part_w)
            piece = dot(hidden[0], wd[:ff, columns]) + dot(hidden[1], wd[ff:, columns])
            for b in range(2):
                kept[delta, b, q * SUB : (q + 1) * SUB, :] = piece[b * SUB : (b + 1) * SUB]
                given[delta, b, q * SUB : (q + 1) * SUB, :] = piece[
                    (b + 2) * SUB : (b + 3) * SUB
                ].astype(BF16)
            fold = (to // SUB == at // extra) & (to % SUB == q * extra + at % extra)
            refolded += dot(jnp.where(fold, 1.0, 0.0).astype(BF16), piece[main:].astype(BF16))
        for b in range(2):
            kept[delta, b, folds * SUB :, :] = refolded[b * SUB : (b + 1) * SUB]
            given[delta, b, folds * SUB :, :] = refolded[(b + 2) * SUB : (b + 3) * SUB].astype(BF16)

    pl.semaphore_wait(barrier, 3)
    pass_on(1)
    lax.fori_loop(0, WINDOW, lambda step, carry: (dispatch(step), carry)[1], 0)
    for copy in remote_w:
        copy.start()

    def body(step, carry):
        @pl.when(step < steps)
        def _():
            delta = delta_of(step)

            @pl.when(delta != 0)
            def _():
                wait_arrival(delta, 0)

            relay(delta, 0).start()
            wait_arrival(delta, 1)
            relay(delta, 1).start()

        @pl.when(step + WINDOW < steps)
        def _():
            dispatch(step + WINDOW)

        @pl.when((step >= 1) & (step <= steps))
        def _():
            delta = delta_of(step - 1)

            @pl.when(step == 1)
            def _():
                for copy in local_w:
                    copy.wait()
                for copy in remote_w:
                    copy.wait_recv()

            for side in range(2):
                relay(delta, side).wait_recv()
            compute(delta)
            give(delta).start()

        @pl.when(step >= 2)
        def _():
            delta = delta_of(step - 2)
            give(delta).wait_recv()

            @pl.when(delta != 0)
            def _():
                final[delta] = (kept[delta] + part[delta].astype(F32)).astype(BF16)
                for side in range(2):
                    send_back(delta, side).start()

            @pl.when(delta == 0)
            def _():
                final[0, 1] = (kept[0, 1] + part[0, 1].astype(F32)).astype(BF16)
                send_back_far().start()
                returned[pair] = (kept[0, 0] + part[0, 0].astype(F32)).astype(BF16)

        return carry

    lax.fori_loop(0, steps + 2, body, 0)

    target[2:4, :] = gates_ref[...]
    weight[...] = target[...].T
    total[...] = jnp.zeros_like(total)

    def wait_return(expert):
        pltpu.make_async_remote_copy(
            final.at[0, 1],
            returned.at[expert],
            r_send.at[0],
            r_recv.at[expert],
            device_id={"ep": mate},
        ).wait_recv()

    def split(value):
        high = value.astype(BF16)
        return [high, (value - high.astype(F32)).astype(BF16)]

    def collect(i, carry):
        near = [delta_of(2 * i), delta_of(2 * i + 1)]
        group = []
        for delta in near:
            group.append(lax.rem(pair + jnp.where(delta == 0, steps, delta), experts))
            group.append(lax.rem(pair - delta + experts, experts))
        count = len(group) * SUB
        column = iota((tok, count), 1)
        row = column % SUB
        first = jnp.zeros((tok, count), jnp.int32)
        for j, expert in enumerate(group):
            first = jnp.where(column // SUB == j, expert * cap, first)
        straight = jnp.zeros((tok, count), F32)
        folded = jnp.zeros((tok, count), F32)
        for k in range(2):
            place, gate = weight[:, k : k + 1], weight[:, k + 2 : k + 3]
            straight = jnp.where(place == (first + row).astype(F32), gate, straight)
            folded = jnp.where(place == (first + SUB + row % extra).astype(F32), gate, folded)
        shares = jnp.concatenate(split(straight), axis=0)
        shares_folded = []
        for q in range(folds):
            shares_folded += split(jnp.where(row // extra == q, folded, 0.0))
        shares_folded = jnp.concatenate(shares_folded, axis=0)

        for j, (delta, expert) in enumerate(zip([near[0], near[0], near[1], near[1]], group)):
            if j % 2 == 0:
                wait_return(expert)
            else:

                @pl.when(delta != 0)
                def _():
                    wait_return(expert)

        def rows_of(q):
            return jnp.concatenate(
                [returned[expert, q * SUB : (q + 1) * SUB, :] for expert in group], axis=0
            )

        more = dot(shares_folded, rows_of(folds))
        for q in range(folds):
            some = dot(shares, rows_of(q))
            part_sum = some[:tok] + some[tok:]
            part_sum += more[2 * q * tok : (2 * q + 1) * tok]
            part_sum += more[(2 * q + 1) * tok : (2 * q + 2) * tok]
            total[:, q * part_w : (q + 1) * part_w] += part_sum
        return carry

    lax.fori_loop(0, steps // 2, collect, 0)
    out_ref[...] = total[...].astype(BF16)

    for copy in remote_w:
        copy.wait_send()

    def drain(delta, carry):
        for side in range(2):
            relay(delta, side).wait_send()
        give(delta).wait_send()

        @pl.when(delta != 0)
        def _():
            for side in range(2):
                send_back(delta, side).wait_send()

        @pl.when(delta == 0)
        def _():
            send_back_far().wait_send()

        return carry

    lax.fori_loop(0, steps, drain, 0)

    def drain_dispatch(i, carry):
        expert = lax.rem(pair + i, experts)
        send_to(expert, 0, 0, 1).wait_send()
        return carry

    lax.fori_loop(1, experts, drain_dispatch, 0)


def per_device(tokens, routing, gates, norm_gain, w_gate, w_up, w_down):
    tok, width = tokens.shape
    top = routing.shape[1]
    ff = w_gate.shape[2]
    devices = lax.axis_size("ep")
    experts = devices // GROUP
    steps = experts // 2
    cap = GROUP * (5 * tok * top // (4 * devices))
    extra = cap - SUB
    folds = SUB // extra
    assert top == 2 and tok == LANES and steps % 2 == 0
    assert 0 < extra and folds * extra == SUB and width % (folds * LANES) == 0
    block = ((folds + 1) * SUB, width // folds)
    batch = 4 * cap
    pairs = (steps, 2) + block
    dma = pltpu.SemaphoreType.DMA
    vmem = pl.BlockSpec(memory_space=pltpu.VMEM)
    hbm = pl.BlockSpec(memory_space=pltpu.HBM)
    return pl.pallas_call(
        functools.partial(layer_kernel, devices, cap),
        out_shape=jax.ShapeDtypeStruct((tok, width), BF16),
        in_specs=[hbm, vmem, vmem, vmem, hbm, hbm, hbm],
        out_specs=vmem,
        scratch_shapes=[
            pltpu.VMEM((2, width, ff), BF16),
            pltpu.VMEM((2, width, ff), BF16),
            pltpu.VMEM((2 * ff, width), BF16),
            pltpu.VMEM((tok, width), BF16),
            pltpu.VMEM((tok, width), BF16),
            pltpu.VMEM((tok, tok), F32),
            pltpu.VMEM((tok, tok), F32),
            pltpu.VMEM((tok, width), F32),
            pltpu.VMEM((experts,) + block, BF16),
            pltpu.VMEM(pairs, BF16),
            pltpu.VMEM(pairs, BF16),
            pltpu.VMEM((batch, width), BF16),
            pltpu.VMEM((2, batch, ff), BF16),
            pltpu.VMEM(pairs, F32),
            pltpu.VMEM(pairs, BF16),
            pltpu.VMEM(pairs, BF16),
            pltpu.VMEM(pairs, BF16),
            pltpu.VMEM((experts,) + block, BF16),
            pltpu.SemaphoreType.REGULAR((devices // 4,)),
            pltpu.SemaphoreType.REGULAR((devices // 4,)),
            dma,
            dma((3,)),
            dma((3,)),
            dma((3,)),
            dma((experts,)),
            dma((experts,)),
            dma((experts,)),
            dma((experts,)),
            dma((steps,)),
            dma((steps,)),
            dma((experts,)),
            dma((experts,)),
        ],
        compiler_params=pltpu.CompilerParams(
            collective_id=0, has_side_effects=True, vmem_limit_bytes=60 * 1024 * 1024
        ),
    )(tokens, routing.T, gates.T, norm_gain.reshape(width // LANES, LANES), w_gate, w_up, w_down)


def solution(mesh):
    placed = (
        P(("grp", "ep"), None),
        P(("grp", "ep"), None),
        P(("grp", "ep"), None),
        P(),
        P("ep", None, None),
        P("ep", None, None),
        P("ep", None, None),
    )
    return jax.shard_map(
        per_device, mesh=mesh, in_specs=placed, out_specs=P(("grp", "ep"), None), check_vma=False
    )
```
